32 devices in a mesh: sp: 16 (over z, y, x), tp: 2 (over core).
Axes of the slice: x: 2, y: 2, z: 4, core: 2. Of those that a mesh axis runs over, the one named last changes fastest.
Arguments:
- head_value_rows: bfloat16 [12288, 2048], P('sp', 'tp'), may hold values from -6 to 6
- entry_map_rows: bfloat16 [12288, 1024], P('sp', 'tp'), may hold values from -6 to 6
- readout_map_rows: bfloat16 [12288, 1024], P('sp', 'tp'), may hold values from -6 to 6
- output_gate_rows: bfloat16 [12288, 2048], P('sp', 'tp'), may hold values from -6 to 6
- step_before_softplus: bfloat16 [12288, 32], P('sp', 'tp'), may hold values from -8 to 8
- sudden_log_decay: float32 [12288, 32], P('sp', 'tp'), may hold values from -1 to 0
- document_index: int32 [12288], replicated, may hold values from 0 to 3, never falling along the last dimension, each value on 1 to 6144 neighbouring positions
- head_rate_logarithm: float32 [2, 32], P(None, 'tp'), may hold values from -30 to 0
- head_step_bias: float32 [2, 32], P(None, 'tp'), may hold values from -3 to 3
- value_conv_taps: bfloat16 [5, 2048], P(None, 'tp'), may hold values from -2.5 to 2.5
- entry_conv_taps: bfloat16 [5, 1024], P(None, 'tp'), may hold values from -2.5 to 2.5
- readout_conv_taps: bfloat16 [5, 1024], P(None, 'tp'), may hold values from -2.5 to 2.5
- group_norm_gain: float32 [2048], P('tp'), may hold values from 0.1 to 1.9
- mixer_output_weight: bfloat16 [2048, 2048], P('tp'), may hold values from -0.125 to 0.125
- stream: bfloat16 [12288, 2048], P('sp', 'tp'), may hold values from -200 to 200
- mixer_norm_gain: float32 [2048], P('tp'), may hold values from 0.1 to 1.9
- channel_norm_gain: float32 [2048], P('tp'), may hold values from 0.1 to 1.9
- up_projection_weight: bfloat16 [2048, 8192], P('sp', 'tp'), may hold values from -0.125 to 0.125
- down_projection_weight: bfloat16 [2048, 8192], P('sp', 'tp'), may hold values from -0.0625 to 0.0625
Outputs:
- mixed: bfloat16 [12288, 2048], P('sp', 'tp')
The draws below stay inside these ranges and needn't reach their ends.
All inputs are finite; a program needn't handle non-finite values.
Results may differ from the reference program's by a relative error of at most 0.018.
Values may be sent and summed in bfloat16 or wider, within the bound.
A program may use at most 128 MiB of HBM per device.

```python
import math
import jax
import jax.numpy as jnp
import numpy as np
from jax import lax

D = 2048
HEADS = 32
HEAD_DIM = 64
GROUPS = 8
STATE = 128
FF = 8192
CONV_WIDTH = 5
BLOCK = 128
TOK_DEV = 768
INNER = 2048
TOKENS = 12288
N_SP = 16
N_TP = 2


def draw_step_before_softplus(key, part):
    jitter_key, shift_key = jax.random.split(key)
    jitter = jnp.clip(jax.random.normal(jitter_key, (TOKENS, HEADS), jnp.float32), -4.0, 4.0)
    shifts = jax.random.uniform(shift_key, (TOKENS // TOK_DEV, 1, HEADS), jnp.float32, -1.0, 1.5)
    shifts = jnp.broadcast_to(shifts, (TOKENS // TOK_DEV, TOK_DEV, HEADS)).reshape(TOKENS, HEADS)
    return (jitter + shifts).astype(jnp.bfloat16)


def draw_head_rate_logarithm(key, part):
    pick_key, slow_key, fast_key = jax.random.split(key, 3)
    quick = jax.random.randint(pick_key, (2, HEADS), 0, 2) == 1
    slow_rate = jax.random.uniform(slow_key, (2, HEADS), jnp.float32, math.log(0.1), math.log(0.5))
    slow_rate = slow_rate - jnp.log(jnp.float32(TOKENS))
    fast_rate = jax.random.uniform(fast_key, (2, HEADS), jnp.float32, math.log(0.01), math.log(1.0 / 30.0))
    return jnp.where(quick, fast_rate, slow_rate)


def draw_sudden_log_decay(key, part):
    where_key, depth_key = jax.random.split(key)
    struck = jax.random.randint(where_key, (TOKENS, 1), 0, TOKENS) < 4
    depth = jax.random.uniform(depth_key, (TOKENS, HEADS), jnp.float32, math.log(0.5), math.log(0.8))
    return jnp.where(struck, depth, 0.0)


def draw_stream(key, part):
    base_key, row_key = jax.random.split(key, 2)
    col_scale = 3.0 ** (jnp.arange(D, dtype=jnp.float32) / D - 0.5)
    values = jnp.clip(jax.random.normal(base_key, (TOKENS, D), jnp.float32), -6.0, 6.0)
    row_scale = jnp.exp(jax.random.uniform(row_key, (TOKENS, 1), jnp.float32, math.log(0.5), math.log(2.0)))
    return (values * row_scale * col_scale).astype(jnp.bfloat16)


def levels(stream_key, shape, cuts, low, largest):
    loudness = 1.0
    for axis_at, blocks in cuts:
        heights = jax.random.uniform(jax.random.fold_in(jax.random.fold_in(stream_key, 6), axis_at), (blocks,), jnp.float32, low / len(cuts), largest / len(cuts))
        loudness = loudness * jnp.repeat(jnp.exp(heights), shape[axis_at] // blocks).reshape((-1,) + (1,) * (len(shape) - 1 - axis_at))
    return loudness


def split_up(amount, total, bound, skew):
    weights = [(1 << 20) // math.isqrt(grade ** skew) + 1 for grade in range(2, amount + 1)]
    spare, holding = total - bound - (amount - 1), [1] * (amount - 1)
    while spare > 0:
        movable = [i for i in range(amount - 1) if holding[i] < bound]
        pool, remaining = sum([weights[i] for i in movable]), spare
        for i in movable:
            more = min(bound - holding[i], max(1, remaining * weights[i] // pool), spare)
            holding[i] = holding[i] + more
            spare = spare - more
    return np.array([bound] + holding)


def ragged_sizes(key, amount, total, reach, skew):
    if amount == 2:
        one = jax.random.randint(key, (), max(1, total - reach), min(reach, total - 1) + 1)
        return jnp.stack([one, total - one])
    sizes = jnp.asarray(split_up(amount, total, reach, skew), jnp.int32)
    twos = (amount - 1) // 2
    donor, receiver = sizes[1:1 + 2 * twos:2], sizes[2:2 + 2 * twos:2]
    margin = jnp.minimum(donor - 1, reach - receiver)
    shifted = jax.random.randint(jax.random.fold_in(key, 1), (twos,), 0, 1 << 20) % (margin + 1)
    sizes = sizes.at[1:1 + 2 * twos:2].set(donor - shifted).at[2:2 + 2 * twos:2].set(receiver + shifted)
    return sizes[jax.random.permutation(jax.random.fold_in(key, 2), amount)]


def noise(own_key, extent, deviation, most, cuts=(), kind=jnp.bfloat16):
    loudness = levels(own_key, extent, cuts, -0.22, 0.18) if cuts else 1.0
    values = jax.random.normal(own_key, extent, jnp.float32) * deviation * loudness
    return jnp.minimum(jnp.maximum(values, -most), most).astype(kind)


def setup_inputs(seed: int = 0) -> dict:
    arg_keys = jax.random.split(jax.random.key(seed), 20)
    return {
        "head_value_rows": noise(arg_keys[0], (TOKENS, INNER), 1.0, 6.0, ((0, 16), (1, 2))),
        "entry_map_rows": noise(arg_keys[1], (TOKENS, GROUPS * STATE), 1.0, 6.0, ((0, 16), (1, 2))),
        "readout_map_rows": noise(arg_keys[2], (TOKENS, GROUPS * STATE), 1.0, 6.0, ((0, 16), (1, 2))),
        "output_gate_rows": noise(arg_keys[3], (TOKENS, INNER), 1.0, 6.0, ((0, 16), (1, 2))),
        "step_before_softplus": draw_step_before_softplus(jax.random.fold_in(arg_keys[19], 71), 0),
        "sudden_log_decay": draw_sudden_log_decay(jax.random.fold_in(arg_keys[19], 71), 0),
        "document_index": jnp.searchsorted(jnp.cumsum(ragged_sizes(arg_keys[6], N_SP // 4, TOKENS, 8 * TOK_DEV, 1)), jnp.arange(TOKENS), side="right").astype(jnp.int32),
        "head_rate_logarithm": draw_head_rate_logarithm(jax.random.fold_in(arg_keys[19], 71), 0),
        "head_step_bias": noise(arg_keys[8], (2, HEADS), 0.5, 3.0, ((1, 2),), jnp.float32),
        "value_conv_taps": noise(arg_keys[9], (CONV_WIDTH, INNER), CONV_WIDTH ** -0.5, 2.5, ((1, 2),)),
        "entry_conv_taps": noise(arg_keys[10], (CONV_WIDTH, GROUPS * STATE), CONV_WIDTH ** -0.5, 2.5, ((1, 2),)),
        "readout_conv_taps": noise(arg_keys[11], (CONV_WIDTH, GROUPS * STATE), CONV_WIDTH ** -0.5, 2.5, ((1, 2),)),
        "group_norm_gain": jnp.clip(1.0 + 0.18 * jax.random.normal(arg_keys[12], (INNER,), jnp.float32), 0.1, 1.9),
        "mixer_output_weight": noise(arg_keys[13], (INNER, D), INNER ** -0.5, 0.125, ((0, 2),)),
        "stream": draw_stream(jax.random.fold_in(arg_keys[19], 71), 0),
        "mixer_norm_gain": jnp.clip(1.0 + 0.18 * jax.random.normal(arg_keys[15], (D,), jnp.float32), 0.1, 1.9),
        "channel_norm_gain": jnp.clip(1.0 + 0.18 * jax.random.normal(arg_keys[16], (D,), jnp.float32), 0.1, 1.9),
        "up_projection_weight": noise(arg_keys[17], (D, FF), D ** -0.5, 0.125, ((0, 16), (1, 2))),
        "down_projection_weight": noise(arg_keys[18], (D, FF), FF ** -0.5, 0.0625, ((0, 16), (1, 2))),
    }


exact_prec = lax.Precision.HIGHEST
norm_eps = 1e-05
resid_scale = 1.4142135623730951

def block_step(running, blocks):
    states, last_doc = running
    scaled, entries, readout, decay_logarithm, block_ids = blocks
    block_len = block_ids.shape[0]
    cum_decay = jnp.cumsum(decay_logarithm, axis=0)
    indices = lax.iota(jnp.int32, block_len)
    linked = (indices[:, None] >= indices[None, :]) & (block_ids[:, None] == block_ids[None, :])
    link_mask = linked[:, :, None, None]
    spread = cum_decay[:, None] - cum_decay[None, :]
    weights = jnp.where(link_mask, jnp.exp(jnp.where(link_mask, spread, 0.0)), 0.0)
    scores = jnp.einsum('tgn,sgn->tsg', readout, entries, precision=exact_prec)
    within = jnp.einsum('tsg,tsgr,sgrp->tgrp', scores, weights, scaled, precision=exact_prec)
    arrival = jnp.where((block_ids == last_doc)[:, None, None], jnp.exp(cum_decay), 0.0)
    carried = jnp.einsum('tgn,grpn->tgrp', readout, states, precision=exact_prec) * arrival[..., None]
    end_doc = block_ids[-1]
    to_end = jnp.where((block_ids == end_doc)[:, None, None], jnp.exp(cum_decay[-1] - cum_decay), 0.0)
    passing = jnp.where(end_doc == last_doc, jnp.exp(cum_decay[-1]), 0.0)
    fresh = jnp.einsum('sgn,sgr,sgrp->grpn', entries, to_end, scaled, precision=exact_prec)
    return ((states * passing[..., None, None] + fresh, end_doc), within + carried)

def sweep_blocks(scaled, entries, readout, decay_logarithm, document_index, states, last_doc, block_len):
    row_count = document_index.shape[0]
    block_count = row_count // block_len

    def in_blocks(array):
        return array.reshape((block_count, block_len) + array.shape[1:])
    inputs = tuple((in_blocks(array) for array in (scaled, entries, readout, decay_logarithm, document_index)))
    (states, last_doc), output = lax.scan(block_step, (states, last_doc), inputs)
    return (output.reshape((row_count,) + output.shape[2:]), states)

def short_conv(inputs, weights, document_index):
    taps = weights.shape[0]
    half_width = taps // 2
    row_count = inputs.shape[0]
    padded = jnp.pad(inputs, ((half_width, half_width), (0, 0)))
    doc_pad = jnp.pad(document_index, half_width, constant_values=-1)
    summed = jnp.zeros(inputs.shape, jnp.float32)
    for offset in range(taps):
        same_doc = (doc_pad[offset:offset + row_count] == document_index)[:, None]
        summed = summed + weights[offset] * jnp.where(same_doc, padded[offset:offset + row_count], 0.0)
    return jax.nn.silu(summed)

def layer_norm(residual, gain):
    row_mean = lax.optimization_barrier(jnp.mean(residual, axis=1))
    row_var = lax.optimization_barrier(jnp.mean(residual * residual, axis=1)) - row_mean * row_mean
    return ((residual - row_mean[:, None]) * lax.rsqrt(row_var + norm_eps)[:, None] * gain).astype(jnp.bfloat16)

def block_sums(left, right):
    parts = jnp.einsum('tjc,jcd->jtd', left, right)
    rounded = parts.astype(jnp.bfloat16)
    rounded = lax.optimization_barrier(rounded)
    return lax.optimization_barrier(jnp.sum(rounded.astype(jnp.float32), axis=0))

def reference(head_value_rows, entry_map_rows, readout_map_rows, output_gate_rows, step_before_softplus, sudden_log_decay, document_index, head_rate_logarithm, head_step_bias, value_conv_taps, entry_conv_taps, readout_conv_taps, group_norm_gain, mixer_output_weight, stream, mixer_norm_gain, channel_norm_gain, up_projection_weight, down_projection_weight):
    per_group = HEADS // GROUPS
    values = short_conv(head_value_rows.astype(jnp.float32), value_conv_taps.astype(jnp.float32), document_index)
    values = values.reshape(TOKENS, GROUPS, per_group, HEAD_DIM)
    entries = short_conv(entry_map_rows.astype(jnp.float32), entry_conv_taps.astype(jnp.float32), document_index)
    entries = entries.reshape(TOKENS, GROUPS, STATE)
    readout = short_conv(readout_map_rows.astype(jnp.float32), readout_conv_taps.astype(jnp.float32), document_index)
    readout = readout.reshape(TOKENS, GROUPS, STATE)
    summed = jnp.zeros((TOKENS, GROUPS, per_group, HEAD_DIM), jnp.float32)
    for sweep_direction in range(2):
        head_step_length = jax.nn.softplus(step_before_softplus.astype(jnp.float32) + head_step_bias[sweep_direction])
        decay_logarithm = -jnp.exp(head_rate_logarithm[sweep_direction]) * head_step_length + sudden_log_decay
        decay_logarithm = decay_logarithm.reshape(TOKENS, GROUPS, per_group)
        scaled = values * head_step_length.reshape(TOKENS, GROUPS, per_group)[..., None]
        arrays = (scaled, entries, readout, decay_logarithm, document_index)
        if sweep_direction == 1:
            arrays = tuple((jnp.flip(array, 0) for array in arrays))
        start_state = jnp.zeros((GROUPS, per_group, HEAD_DIM, STATE), jnp.float32)
        output, _ = sweep_blocks(*arrays, start_state, jnp.int32(-1), BLOCK)
        if sweep_direction == 1:
            output = jnp.flip(output, 0)
        summed = summed + output
    gated = summed.reshape(TOKENS, GROUPS, per_group * HEAD_DIM)
    gated = gated * jax.nn.silu(output_gate_rows.astype(jnp.float32)).reshape(TOKENS, GROUPS, per_group * HEAD_DIM)
    gated = gated * lax.rsqrt(lax.optimization_barrier(jnp.mean(gated * gated, axis=2, keepdims=True)) + norm_eps)
    normed = (gated.reshape(TOKENS, INNER) * group_norm_gain).astype(jnp.bfloat16)
    out_blocks = mixer_output_weight.astype(jnp.float32).reshape(N_TP, INNER // N_TP, D)
    down_blocks = down_projection_weight.astype(jnp.float32).reshape(D, N_TP, FF // N_TP)

    def dense_rows(pieces):
        normed_rows, stream_rows = pieces
        mixer_sum = block_sums(normed_rows.astype(jnp.float32).reshape(-1, N_TP, INNER // N_TP), out_blocks)
        first_sum = resid_scale * stream_rows.astype(jnp.float32) + mixer_sum
        normed_one = layer_norm(first_sum, mixer_norm_gain)
        hidden = jnp.dot(normed_one, up_projection_weight, preferred_element_type=jnp.float32)
        squared = jnp.square(jax.nn.relu(hidden)).astype(jnp.bfloat16)
        parts = jnp.einsum('tjf,djf->jtd', squared.astype(jnp.float32).reshape(-1, N_TP, FF // N_TP), down_blocks)
        rounded = lax.optimization_barrier(parts.astype(jnp.bfloat16))
        down_sum = lax.optimization_barrier(jnp.sum(rounded.astype(jnp.float32), axis=0))
        second_sum = resid_scale * normed_one.astype(jnp.float32) + down_sum
        return layer_norm(second_sum, channel_norm_gain)
    result = lax.map(dense_rows, (normed.reshape(N_SP, TOK_DEV, INNER), stream.reshape(N_SP, TOK_DEV, D)))
    return result.reshape(TOKENS, D)
```

```python
import jax
import jax.numpy as jnp
from jax import lax
from jax.sharding import PartitionSpec as P

HEAD_DIM = 64
STATE = 128
BLOCK = 128
LONGEST_DOCUMENT = 6144


exact_prec = lax.Precision.HIGHEST
norm_eps = 1e-05
resid_scale = 1.4142135623730951
bf16 = jnp.bfloat16
f32 = jnp.float32


def swap(array):
    return lax.ppermute(array, "tp", [(0, 1), (1, 0)])


def tp_scatter(partial):
    if lax.axis_size("tp") != 2:
        return lax.psum_scatter(
            partial.astype(bf16), "tp", scatter_dimension=1, tiled=True
        ).astype(f32)
    me = lax.axis_index("tp")
    width = partial.shape[1] // 2
    rounded = partial.astype(bf16)
    other = lax.dynamic_slice_in_dim(rounded, (1 - me) * width, width, 1)
    mine = lax.dynamic_slice_in_dim(rounded, me * width, width, 1)
    return mine.astype(f32) + swap(other).astype(f32)


def tp_gather(array):
    if lax.axis_size("tp") != 2:
        return lax.all_gather(array, "tp", axis=1, tiled=True)
    other = swap(array)
    first = lax.axis_index("tp") == 0
    return jnp.concatenate(
        [jnp.where(first, array, other), jnp.where(first, other, array)], axis=1
    )


def norm_rows(residual, gain, width):
    sums = jnp.stack([jnp.sum(residual, axis=1), jnp.sum(residual * residual, axis=1)])
    if lax.axis_size("tp") == 2:
        sums = sums + swap(sums)
    else:
        sums = lax.psum(sums, "tp")
    row_mean = sums[0] / width
    row_var = sums[1] / width - row_mean * row_mean
    return ((residual - row_mean[:, None]) * lax.rsqrt(row_var + norm_eps)[:, None] * gain).astype(
        bf16
    )


def shifted(array, step):
    count = lax.axis_size("sp")
    if step > 0:
        pairs = [(i, i + step) for i in range(count - step)]
    else:
        pairs = [(i, i + step) for i in range(-step, count)]
    return lax.ppermute(array, "sp", pairs)


def incoming_state(end_state, passing_all, direction, reach):
    count = lax.axis_size("sp")
    place = lax.axis_index("sp")
    state = shifted(end_state.astype(bf16), direction).astype(f32)
    source = place - direction
    inside = (source >= 0) & (source < count)
    through = jnp.where(
        inside,
        lax.dynamic_index_in_dim(passing_all, jnp.clip(source, 0, count - 1), 0, False),
        0.0,
    )
    covered = 1
    while covered < min(reach, count - 1):
        state = state + through[..., None, None] * shifted(
            state.astype(bf16), direction * covered
        ).astype(f32)
        for more in range(covered, 2 * covered):
            source = place - direction * (more + 1)
            inside = (source >= 0) & (source < count)
            through = through * jnp.where(
                inside,
                lax.dynamic_index_in_dim(passing_all, jnp.clip(source, 0, count - 1), 0, False),
                0.0,
            )
        covered *= 2
    return state


def per_device(
    head_value_rows,
    entry_map_rows,
    readout_map_rows,
    output_gate_rows,
    step_before_softplus,
    sudden_log_decay,
    document_index,
    head_rate_logarithm,
    head_step_bias,
    value_conv_taps,
    entry_conv_taps,
    readout_conv_taps,
    group_norm_gain,
    mixer_output_weight,
    stream,
    mixer_norm_gain,
    channel_norm_gain,
    up_projection_weight,
    down_projection_weight,
):
    up_full = lax.all_gather(up_projection_weight, "sp", axis=0, tiled=True)
    down_full = lax.all_gather(down_projection_weight, "sp", axis=0, tiled=True)

    rows = head_value_rows.shape[0]
    heads = step_before_softplus.shape[1]
    groups = entry_map_rows.shape[1] // STATE
    per_group = heads // groups
    value_width = head_value_rows.shape[1]
    state_width = entry_map_rows.shape[1]
    model_width = mixer_output_weight.shape[1]
    blocks = rows // BLOCK
    sp_count = lax.axis_size("sp")
    place = lax.axis_index("sp")
    position = place * rows

    taps = value_conv_taps.shape[0]
    half = taps // 2
    ends = jnp.concatenate(
        [
            jnp.concatenate([a[rows - half :], a[:half]], axis=0)
            for a in (head_value_rows, entry_map_rows, readout_map_rows)
        ],
        axis=1,
    )
    low_all = shifted(ends[:half], 1)
    high_all = shifted(ends[half:], -1)
    doc_pad = jnp.pad(document_index, half + 1, constant_values=-1)
    window_ids = lax.dynamic_slice_in_dim(doc_pad, position + 1, rows + 2 * half)
    own_ids = window_ids[half : half + rows]
    prev_id = window_ids[half - 1]
    next_id = window_ids[half + rows]

    def conv(array, weights, start):
        width = array.shape[1]
        extended = jnp.concatenate(
            [low_all[:, start : start + width], array, high_all[:, start : start + width]], axis=0
        )
        weights = weights.astype(f32)
        total = weights[half] * array.astype(f32)
        for offset in range(taps):
            if offset == half:
                continue
            same = (window_ids[offset : offset + rows] == own_ids)[:, None]
            total = total + weights[offset] * jnp.where(
                same, extended[offset : offset + rows].astype(f32), 0.0
            )
        return jax.nn.silu(total).astype(bf16)

    values = conv(head_value_rows, value_conv_taps, 0)
    entries = conv(entry_map_rows, entry_conv_taps, value_width)
    readout = conv(readout_map_rows, readout_conv_taps, value_width + state_width)
    values = values.reshape(blocks, BLOCK, groups, per_group, HEAD_DIM)
    entries = entries.reshape(blocks, BLOCK, groups, STATE)
    readout = readout.reshape(blocks, BLOCK, groups, STATE)

    raw = step_before_softplus.astype(f32).T
    steps = jax.nn.softplus(raw[None] + head_step_bias[:, :, None])
    decay = -jnp.exp(head_rate_logarithm)[:, :, None] * steps + sudden_log_decay.T[None]
    shape = (2, groups, per_group, blocks, BLOCK)
    steps = jnp.transpose(steps.reshape(shape), (0, 3, 1, 2, 4))
    decay = jnp.transpose(decay.reshape(shape), (0, 3, 1, 2, 4))
    at = lax.iota(jnp.int32, BLOCK)
    upto = (at[:, None] <= at[None, :]).astype(f32)
    running = jnp.einsum("kbgrs,st->kbgrt", decay, upto, precision=exact_prec)
    totals = running[..., -1]
    ahead = running[0]
    behind = running[1] - decay[1]

    ids = own_ids.reshape(blocks, BLOCK)
    first_ids, last_ids = ids[:, 0], ids[:, -1]
    before = jnp.concatenate([prev_id[None], last_ids[:-1]])
    after = jnp.concatenate([first_ids[1:], next_id[None]])
    pass_f = jnp.where((before == last_ids)[:, None, None], jnp.exp(totals[0]), 0.0)
    pass_b = jnp.where((after == first_ids)[:, None, None], jnp.exp(totals[1]), 0.0)
    end_f = jnp.where(
        (ids == last_ids[:, None])[:, None, None], jnp.exp(totals[0][..., None] - ahead), 0.0
    ) * steps[0]
    end_b = jnp.where((ids == first_ids[:, None])[:, None, None], jnp.exp(behind), 0.0) * steps[1]
    arrive_f = jnp.where((ids == before[:, None])[:, None, None], jnp.exp(ahead), 0.0)
    arrive_b = jnp.where(
        (ids == after[:, None])[:, None, None], jnp.exp(totals[1][..., None] - behind), 0.0
    )

    own_pass = jnp.stack([jnp.prod(pass_f, axis=0), jnp.prod(pass_b, axis=0)])
    pass_all = lax.all_gather(own_pass, "sp")

    def fresh_states(weight):
        weighted = values.astype(f32) * jnp.transpose(weight, (0, 3, 1, 2))[..., None]
        return jnp.einsum(
            "bsgrp,bsgn->bgrpn", weighted.astype(bf16), entries, preferred_element_type=f32
        )

    fresh_f = fresh_states(end_f)
    fresh_b = fresh_states(end_b)

    end_state = fresh_f[0]
    for b in range(1, blocks):
        end_state = end_state * pass_f[b][..., None, None] + fresh_f[b]
    start_state = fresh_b[blocks - 1]
    for b in range(blocks - 2, -1, -1):
        start_state = start_state * pass_b[b][..., None, None] + fresh_b[b]
    reach = -(-LONGEST_DOCUMENT // rows)
    in_f = incoming_state(end_state, pass_all[:, 0], 1, reach)
    in_b = incoming_state(start_state, pass_all[:, 1], -1, reach)

    scores = jnp.einsum("btgn,bsgn->bgts", readout, entries, preferred_element_type=f32)
    later = at[:, None] > at[None, :]
    equal = at[:, None] == at[None, :]
    linked = (ids[:, :, None] == ids[:, None, :])[:, None, None]
    spread = jnp.where(
        later,
        ahead[..., :, None] - ahead[..., None, :],
        behind[..., None, :] - behind[..., :, None],
    )
    strength = jnp.where(
        later,
        steps[0][..., None, :],
        jnp.where(equal, steps[0][..., None, :], 0.0) + steps[1][..., None, :],
    )
    weights = jnp.where(linked, jnp.exp(spread) * strength, 0.0)
    mixing = (scores[:, :, None] * weights).astype(bf16)
    output = jnp.einsum("bgrts,bsgrp->bgrtp", mixing, values, preferred_element_type=f32)

    state_f = [in_f]
    for b in range(blocks - 1):
        state_f.append(state_f[-1] * pass_f[b][..., None, None] + fresh_f[b])
    state_b = [in_b]
    for b in range(blocks - 1, 0, -1):
        state_b.append(state_b[-1] * pass_b[b][..., None, None] + fresh_b[b])
    entering_f = jnp.stack([s.astype(bf16) for s in state_f])
    entering_b = jnp.stack([s.astype(bf16) for s in state_b[::-1]])
    carried_f = jnp.einsum("btgn,bgrpn->bgrtp", readout, entering_f, preferred_element_type=f32)
    carried_b = jnp.einsum("btgn,bgrpn->bgrtp", readout, entering_b, preferred_element_type=f32)
    output = output + carried_f * arrive_f[..., None] + carried_b * arrive_b[..., None]

    gated = jnp.transpose(output, (0, 3, 1, 2, 4)).reshape(rows, groups, per_group * HEAD_DIM)
    gated = gated * jax.nn.silu(output_gate_rows.astype(f32)).reshape(gated.shape)
    gated = gated * lax.rsqrt(jnp.mean(gated * gated, axis=2, keepdims=True) + norm_eps)
    normed = (gated.reshape(rows, value_width) * group_norm_gain).astype(bf16)

    mixer_sum = tp_scatter(jnp.dot(normed, mixer_output_weight, preferred_element_type=f32))
    first_sum = resid_scale * stream.astype(f32) + mixer_sum
    normed_one = norm_rows(first_sum, mixer_norm_gain, model_width)
    hidden = jnp.dot(tp_gather(normed_one), up_full, preferred_element_type=f32)
    squared = jnp.square(jax.nn.relu(hidden)).astype(bf16)
    down_part = lax.dot_general(
        squared, down_full, (((1,), (1,)), ((), ())), preferred_element_type=f32
    )
    second_sum = resid_scale * normed_one.astype(f32) + tp_scatter(down_part)
    return norm_rows(second_sum, channel_norm_gain, model_width)


def solution(mesh):
    placed = (
        P("sp", "tp"),
        P("sp", "tp"),
        P("sp", "tp"),
        P("sp", "tp"),
        P("sp", "tp"),
        P("sp", "tp"),
        P(),
        P(None, "tp"),
        P(None, "tp"),
        P(None, "tp"),
        P(None, "tp"),
        P(None, "tp"),
        P("tp"),
        P("tp", None),
        P("sp", "tp"),
        P("tp"),
        P("tp"),
        P("sp", "tp"),
        P("sp", "tp"),
    )
    return jax.shard_map(
        per_device, mesh=mesh, in_specs=placed, out_specs=P("sp", "tp"), check_vma=False
    )
```

```python
import jax
import jax.numpy as jnp
from jax import lax
from jax.sharding import PartitionSpec as P

HEAD_DIM = 64
STATE = 128
BLOCK = 128
LONGEST_DOCUMENT = 6144
PIECES = 2


exact_prec = lax.Precision.HIGHEST
norm_eps = 1e-05
resid_scale = 1.4142135623730951
bf16 = jnp.bfloat16
f32 = jnp.float32


def swap(array):
    return lax.ppermute(array, "tp", [(0, 1), (1, 0)])


def tp_scatter(partial):
    if lax.axis_size("tp") != 2:
        return lax.psum_scatter(
            partial.astype(bf16), "tp", scatter_dimension=1, tiled=True
        ).astype(f32)
    me = lax.axis_index("tp")
    width = partial.shape[1] // 2
    rounded = partial.astype(bf16)
    other = lax.dynamic_slice_in_dim(rounded, (1 - me) * width, width, 1)
    mine = lax.dynamic_slice_in_dim(rounded, me * width, width, 1)
    return mine.astype(f32) + swap(other).astype(f32)


def tp_gather(array):
    if lax.axis_size("tp") != 2:
        return lax.all_gather(array, "tp", axis=1, tiled=True)
    other = swap(array)
    first = lax.axis_index("tp") == 0
    return jnp.concatenate(
        [jnp.where(first, array, other), jnp.where(first, other, array)], axis=1
    )


def norm_rows(residual, gain, width):
    sums = jnp.stack([jnp.sum(residual, axis=1), jnp.sum(residual * residual, axis=1)])
    if lax.axis_size("tp") == 2:
        sums = sums + swap(sums)
    else:
        sums = lax.psum(sums, "tp")
    row_mean = sums[0] / width
    row_var = sums[1] / width - row_mean * row_mean
    return ((residual - row_mean[:, None]) * lax.rsqrt(row_var + norm_eps)[:, None] * gain).astype(
        bf16
    )


def pair_swap(array):
    count = lax.axis_size("sp")
    return lax.ppermute(array, "sp", [(i, i ^ 1) for i in range(count)])


def pair_weights(weight):
    count = lax.axis_size("sp")
    odd = lax.axis_index("sp") % 2
    width = weight.shape[1] // 2
    mine = lax.dynamic_slice_in_dim(weight, odd * width, width, 1)
    other = pair_swap(lax.dynamic_slice_in_dim(weight, (1 - odd) * width, width, 1))
    both = jnp.concatenate(
        [jnp.where(odd == 0, mine, other), jnp.where(odd == 0, other, mine)], axis=0
    )
    members = [list(range(0, count, 2)), list(range(1, count, 2))]
    return lax.all_gather(both, "sp", axis=0, tiled=True, axis_index_groups=members)


def channel_mixer(rows, up, down):
    hidden = jnp.dot(tp_gather(rows), up, preferred_element_type=f32)
    squared = jnp.square(jax.nn.relu(hidden)).astype(bf16)
    part = lax.dot_general(squared, down, (((1,), (1,)), ((), ())), preferred_element_type=f32)
    return tp_scatter(part)


def shifted(array, step):
    count = lax.axis_size("sp")
    if step > 0:
        pairs = [(i, i + step) for i in range(count - step)]
    else:
        pairs = [(i, i + step) for i in range(-step, count)]
    return lax.ppermute(array, "sp", pairs)


def incoming_state(end_state, passing_all, direction, reach):
    count = lax.axis_size("sp")
    place = lax.axis_index("sp")
    state = shifted(end_state.astype(bf16), direction).astype(f32)
    source = place - direction
    inside = (source >= 0) & (source < count)
    through = jnp.where(
        inside,
        lax.dynamic_index_in_dim(passing_all, jnp.clip(source, 0, count - 1), 0, False),
        0.0,
    )
    covered = 1
    while covered < min(reach, count - 1):
        state = state + through[..., None, None] * shifted(
            state.astype(bf16), direction * covered
        ).astype(f32)
        for more in range(covered, 2 * covered):
            source = place - direction * (more + 1)
            inside = (source >= 0) & (source < count)
            through = through * jnp.where(
                inside,
                lax.dynamic_index_in_dim(passing_all, jnp.clip(source, 0, count - 1), 0, False),
                0.0,
            )
        covered *= 2
    return state


def per_device(
    head_value_rows,
    entry_map_rows,
    readout_map_rows,
    output_gate_rows,
    step_before_softplus,
    sudden_log_decay,
    document_index,
    head_rate_logarithm,
    head_step_bias,
    value_conv_taps,
    entry_conv_taps,
    readout_conv_taps,
    group_norm_gain,
    mixer_output_weight,
    stream,
    mixer_norm_gain,
    channel_norm_gain,
    up_projection_weight,
    down_projection_weight,
):
    up_half, down_half = pair_weights(up_projection_weight), pair_weights(down_projection_weight)

    rows = head_value_rows.shape[0]
    heads = step_before_softplus.shape[1]
    groups = entry_map_rows.shape[1] // STATE
    per_group = heads // groups
    value_width = head_value_rows.shape[1]
    state_width = entry_map_rows.shape[1]
    model_width = mixer_output_weight.shape[1]
    blocks = rows // BLOCK
    sp_count = lax.axis_size("sp")
    place = lax.axis_index("sp")
    position = place * rows

    taps = value_conv_taps.shape[0]
    half = taps // 2
    ends = jnp.concatenate(
        [
            jnp.concatenate([a[rows - half :], a[:half]], axis=0)
            for a in (head_value_rows, entry_map_rows, readout_map_rows)
        ],
        axis=1,
    )
    low_all = shifted(ends[:half], 1)
    high_all = shifted(ends[half:], -1)
    doc_pad = jnp.pad(document_index, half + 1, constant_values=-1)
    window_ids = lax.dynamic_slice_in_dim(doc_pad, position + 1, rows + 2 * half)
    own_ids = window_ids[half : half + rows]
    prev_id = window_ids[half - 1]
    next_id = window_ids[half + rows]

    def conv(array, weights, start):
        width = array.shape[1]
        extended = jnp.concatenate(
            [low_all[:, start : start + width], array, high_all[:, start : start + width]], axis=0
        )
        weights = weights.astype(f32)
        total = weights[half] * array.astype(f32)
        for offset in range(taps):
            if offset == half:
                continue
            same = (window_ids[offset : offset + rows] == own_ids)[:, None]
            total = total + weights[offset] * jnp.where(
                same, extended[offset : offset + rows].astype(f32), 0.0
            )
        return jax.nn.silu(total).astype(bf16)

    values = conv(head_value_rows, value_conv_taps, 0)
    entries = conv(entry_map_rows, entry_conv_taps, value_width)
    readout = conv(readout_map_rows, readout_conv_taps, value_width + state_width)
    values = values.reshape(blocks, BLOCK, groups, per_group, HEAD_DIM)
    entries = entries.reshape(blocks, BLOCK, groups, STATE)
    readout = readout.reshape(blocks, BLOCK, groups, STATE)

    raw = step_before_softplus.astype(f32).T
    steps = jax.nn.softplus(raw[None] + head_step_bias[:, :, None])
    decay = -jnp.exp(head_rate_logarithm)[:, :, None] * steps + sudden_log_decay.T[None]
    shape = (2, groups, per_group, blocks, BLOCK)
    steps = jnp.transpose(steps.reshape(shape), (0, 3, 1, 2, 4))
    decay = jnp.transpose(decay.reshape(shape), (0, 3, 1, 2, 4))
    at = lax.iota(jnp.int32, BLOCK)
    upto = (at[:, None] <= at[None, :]).astype(f32)
    running = jnp.einsum("kbgrs,st->kbgrt", decay, upto, precision=exact_prec)
    totals = running[..., -1]
    ahead = running[0]
    behind = running[1] - decay[1]

    ids = own_ids.reshape(blocks, BLOCK)
    first_ids, last_ids = ids[:, 0], ids[:, -1]
    before = jnp.concatenate([prev_id[None], last_ids[:-1]])
    after = jnp.concatenate([first_ids[1:], next_id[None]])
    pass_f = jnp.where((before == last_ids)[:, None, None], jnp.exp(totals[0]), 0.0)
    pass_b = jnp.where((after == first_ids)[:, None, None], jnp.exp(totals[1]), 0.0)
    end_f = jnp.where(
        (ids == last_ids[:, None])[:, None, None], jnp.exp(totals[0][..., None] - ahead), 0.0
    ) * steps[0]
    end_b = jnp.where((ids == first_ids[:, None])[:, None, None], jnp.exp(behind), 0.0) * steps[1]
    arrive_f = jnp.where((ids == before[:, None])[:, None, None], jnp.exp(ahead), 0.0)
    arrive_b = jnp.where(
        (ids == after[:, None])[:, None, None], jnp.exp(totals[1][..., None] - behind), 0.0
    )

    own_pass = jnp.stack([jnp.prod(pass_f, axis=0), jnp.prod(pass_b, axis=0)])
    pass_all = lax.all_gather(own_pass, "sp")

    def fresh_states(weight):
        weighted = values.astype(f32) * jnp.transpose(weight, (0, 3, 1, 2))[..., None]
        return jnp.einsum(
            "bsgrp,bsgn->bgrpn", weighted.astype(bf16), entries, preferred_element_type=f32
        )

    fresh_f = fresh_states(end_f)
    fresh_b = fresh_states(end_b)

    end_state = fresh_f[0]
    for b in range(1, blocks):
        end_state = end_state * pass_f[b][..., None, None] + fresh_f[b]
    start_state = fresh_b[blocks - 1]
    for b in range(blocks - 2, -1, -1):
        start_state = start_state * pass_b[b][..., None, None] + fresh_b[b]
    reach = -(-LONGEST_DOCUMENT // rows)
    in_f = incoming_state(end_state, pass_all[:, 0], 1, reach)
    in_b = incoming_state(start_state, pass_all[:, 1], -1, reach)

    scores = jnp.einsum("btgn,bsgn->bgts", readout, entries, preferred_element_type=f32)
    later = at[:, None] > at[None, :]
    equal = at[:, None] == at[None, :]
    linked = (ids[:, :, None] == ids[:, None, :])[:, None, None]
    spread = jnp.where(
        later,
        ahead[..., :, None] - ahead[..., None, :],
        behind[..., None, :] - behind[..., :, None],
    )
    strength = jnp.where(
        later,
        steps[0][..., None, :],
        jnp.where(equal, steps[0][..., None, :], 0.0) + steps[1][..., None, :],
    )
    weights = jnp.where(linked, jnp.exp(spread) * strength, 0.0)
    mixing = (scores[:, :, None] * weights).astype(bf16)
    output = jnp.einsum("bgrts,bsgrp->bgrtp", mixing, values, preferred_element_type=f32)

    state_f = [in_f]
    for b in range(blocks - 1):
        state_f.append(state_f[-1] * pass_f[b][..., None, None] + fresh_f[b])
    state_b = [in_b]
    for b in range(blocks - 1, 0, -1):
        state_b.append(state_b[-1] * pass_b[b][..., None, None] + fresh_b[b])
    entering_f = jnp.stack([s.astype(bf16) for s in state_f])
    entering_b = jnp.stack([s.astype(bf16) for s in state_b[::-1]])
    carried_f = jnp.einsum("btgn,bgrpn->bgrtp", readout, entering_f, preferred_element_type=f32)
    carried_b = jnp.einsum("btgn,bgrpn->bgrtp", readout, entering_b, preferred_element_type=f32)
    output = output + carried_f * arrive_f[..., None] + carried_b * arrive_b[..., None]

    gated = jnp.transpose(output, (0, 3, 1, 2, 4)).reshape(rows, groups, per_group * HEAD_DIM)
    gated = gated * jax.nn.silu(output_gate_rows.astype(f32)).reshape(gated.shape)
    gated = gated * lax.rsqrt(jnp.mean(gated * gated, axis=2, keepdims=True) + norm_eps)
    normed = (gated.reshape(rows, value_width) * group_norm_gain).astype(bf16)

    mixer_sum = tp_scatter(jnp.dot(normed, mixer_output_weight, preferred_element_type=f32))
    first_sum = resid_scale * stream.astype(f32) + mixer_sum
    normed_one = norm_rows(first_sum, mixer_norm_gain, model_width)
    piece = rows // PIECES
    returned = [
        pair_swap(
            channel_mixer(
                pair_swap(normed_one[i * piece : (i + 1) * piece]), up_half, down_half
            ).astype(bf16)
        )
        for i in range(PIECES)
    ]
    down_sum = channel_mixer(normed_one, up_half, down_half) + jnp.concatenate(returned).astype(f32)
    second_sum = resid_scale * normed_one.astype(f32) + down_sum
    return norm_rows(second_sum, channel_norm_gain, model_width)


def solution(mesh):
    placed = (
        P("sp", "tp"),
        P("sp", "tp"),
        P("sp", "tp"),
        P("sp", "tp"),
        P("sp", "tp"),
        P("sp", "tp"),
        P(),
        P(None, "tp"),
        P(None, "tp"),
        P(None, "tp"),
        P(None, "tp"),
        P(None, "tp"),
        P("tp"),
        P("tp", None),
        P("sp", "tp"),
        P("tp"),
        P("tp"),
        P("sp", "tp"),
        P("sp", "tp"),
    )
    return jax.shard_map(
        per_device, mesh=mesh, in_specs=placed, out_specs=P("sp", "tp"), check_vma=False
    )
```
